32 devices in a mesh: ep: 8 (over z, x), tp: 4 (over y, core).
Axes of the slice: x: 2, y: 2, z: 4, core: 2. Of those that a mesh axis runs over, the one named last changes fastest.
Arguments:
- tokens: bfloat16 [192, 3072], P('ep'), may hold values from -6 to 6
- norm_gain: float32 [3072], replicated, may hold values from 0.1 to 1.9
- routing: int32 [192, 4], P('ep'), may hold values from 0 to 7, all different within a row; in each aligned block of 24 rows (0 to 23, 24 to 47, ...) at most 13 rows name the same one
- route_weight: float32 [192, 4], P('ep'), may hold values from 0.05 to 1
- w_gate: bfloat16 [8, 3072, 3072], P('ep', None, 'tp'), may hold values from -0.3125 to 0.3125
- w_up: bfloat16 [8, 3072, 3072], P('ep', None, 'tp'), may hold values from -0.3125 to 0.3125
- w_down: bfloat16 [8, 3072, 3072], P('ep', 'tp'), may hold values from -0.01953125 to 0.01953125
Outputs:
- mixed: bfloat16 [192, 3072], P('ep', 'tp')
The draws below stay inside these ranges and needn't reach their ends.
Inputs may be any that keep to these rules, and one draw needn't show every extreme that they name: `routing`: each row names 4 different experts. Within the rows of one device (aligned blocks of 24 rows) no expert is named by more than 13 rows, a bound that some block reaches.
All inputs are finite; a program needn't handle non-finite values.
Results may differ from the reference program's by a relative error of at most 0.019.
Values may be sent and summed in bfloat16 or wider, within the bound.
A program may use at most 64 MiB of HBM per device.

```python
import math
import jax
import jax.numpy as jnp
import numpy as np
from jax import lax

D = 3072
FF = 3072
TOP_K = 4
TOK_DEV = 24
EXPERTS = 8
CAP = 13
TOKENS = 192
N_EP = 8
N_TP = 4


def strengthened(result, own_key, source, target, parts, factor):
    owner, partner = [(jnp.arange(result.shape[dim]) // (result.shape[dim] // parts)).reshape([-1 if axis == dim else 1 for axis in range(result.ndim)]) for dim in (source, target)]
    chosen = jax.random.permutation(own_key, parts)[partner]
    strong = (owner == chosen) | (owner == (partner + parts // 2) % parts)
    return jnp.where(strong, factor * result, result)


def level_of(key, extent, split, smallest, high):
    loudness, own = 1.0, jax.random.fold_in(key, 6)
    for axis_at, parts in split:
        draws = jnp.exp(jax.random.uniform(jax.random.fold_in(own, axis_at), (parts,), jnp.float32, smallest / len(split), high / len(split)))
        loudness = loudness * jnp.repeat(draws, extent[axis_at] // parts).reshape([-1 if axis == axis_at else 1 for axis in range(len(extent))])
    return loudness


def routed_block(own_key, own, number, rows, count, top, limit, slope):
    sequence = jax.random.permutation(own_key, count)
    crowded, ordinary = load_shares(count, rows * top, limit, slope, True), load_shares(count, rows * top, limit, slope, False)
    places = jnp.arange(count)

    def named(sizes, turn):
        used = int((sizes > 0).sum())
        fixed = max(1, used // 4)
        passed = fixed + (places - fixed + turn * (used - fixed)) % max(1, count - fixed)
        return jnp.zeros((count,), jnp.int32).at[sequence[jnp.where(places < fixed, places, passed)]].set(jnp.asarray(sizes, jnp.int32))

    sizes = jnp.where(number % 4 == 0, named(crowded, number // 4), named(ordinary, number - number // 4 - 1))
    mixed = jax.random.permutation(jax.random.fold_in(own, 3), count)
    giver, taker = mixed[0:count // 2 * 2:2], mixed[1:count // 2 * 2:2]
    room = jnp.minimum(sizes[giver] - 1, limit - sizes[taker]) // 2
    room = jnp.where((giver == sequence[0]) | (taker == sequence[0]) | (sizes[taker] == 0), 0, jnp.maximum(room, 0))
    passed = jax.random.randint(jax.random.fold_in(own, 4), (count // 2,), 0, 1 << 20) % (room + 1)
    sizes = sizes.at[giver].add(-passed).at[taker].add(passed)
    labels = jnp.searchsorted(jnp.cumsum(sizes), jnp.arange(rows * top), side="right").astype(jnp.int32)
    grid = labels.reshape(top, rows).T
    grid = grid[jax.random.permutation(jax.random.fold_in(own, 1), rows)]
    turn = jax.random.randint(jax.random.fold_in(own, 2), (rows, 1), 0, top)
    return jnp.take_along_axis(grid, (jnp.arange(top)[None, :] + turn) % top, axis=1)


def load_shares(count, total, reach, lean, full):
    portions = [(1 << 20) // math.isqrt(grade ** lean) + 1 for grade in range(1, count + 1)]
    largest = reach if full else min(reach, max(-(-total // count), total * portions[0] // sum(portions)))
    least = 1 if total - largest >= count - 1 else 0
    counts, surplus = [largest] + [least] * (count - 1), total - largest - least * (count - 1)
    while surplus > 0:
        movable = [i for i in range(1, count) if counts[i] < largest] or [i for i in range(1, count) if counts[i] < reach]
        mass, budget = sum([portions[i] for i in movable]), surplus
        for i in movable:
            addition = min(reach - counts[i], max(1, budget * portions[i] // mass), surplus)
            counts[i] = counts[i] + addition
            surplus = surplus - addition
    return np.array(counts)


def scatter_about(own_key, shape, width, limit, split=(), kind=jnp.bfloat16):
    drawn = jax.random.normal(own_key, shape, jnp.float32) * width
    if len(split) > 0:
        drawn = level_of(own_key, shape, split, -0.22, 0.18) * drawn
    return jnp.clip(drawn, min=-limit, max=limit).astype(kind)


def bell_draw_with(rng, dims, deviation, limit, pieces, heavy, kind=jnp.bfloat16):
    entries = deviation * jax.random.normal(rng, dims, jnp.float32)
    if pieces:
        entries = entries * level_of(rng, dims, pieces, -0.22, 0.18)
    return jnp.clip(strengthened(entries, jax.random.fold_in(rng, 3), *heavy), -limit, limit).astype(kind)


def setup_inputs(seed: int = 0) -> dict:
    streams_of = jax.random.split(jax.random.key(seed), 8)
    tokens = scatter_about(streams_of[0], (TOKENS, D), 1.0, 6.0, ((0, 8),))
    norm_gain = jnp.clip(1.0 + 0.18 * jax.random.normal(streams_of[1], (D,), jnp.float32), 0.1, 1.9)
    routing_keys = jax.random.split(jax.random.fold_in(streams_of[2], 1), TOKENS // TOK_DEV)
    routing_turns = jax.random.permutation(jax.random.fold_in(streams_of[2], 3), TOKENS // TOK_DEV)
    routing = jax.vmap(lambda own, number: routed_block(jax.random.fold_in(streams_of[2], 2), own, number, TOK_DEV, EXPERTS, TOP_K, CAP, 2))(routing_keys, routing_turns).reshape((TOKENS, TOP_K))
    route_weight = jnp.clip(jnp.exp(math.log(1.0) - 2.9957323 * jax.random.uniform(streams_of[3], (TOKENS, TOP_K), jnp.float32) ** level_of(streams_of[3], (TOKENS, TOP_K), ((0, 8),), -0.2, 0.2)), 0.05, 1.0)
    w_gate = scatter_about(streams_of[4], (EXPERTS, D, FF), (D // 9) ** -0.5, 0.3125, ((0, 8), (2, 4)))
    w_up = scatter_about(streams_of[5], (EXPERTS, D, FF), (D // 9) ** -0.5, 0.3125, ((0, 8), (2, 4)))
    w_down = bell_draw_with(streams_of[6], (EXPERTS, FF, D), (64 * FF) ** -0.5, 0.01953125, ((0, 8), (1, 4)), (1, 2, 4, 2.0))
    return {"tokens": tokens, "norm_gain": norm_gain, "routing": routing, "route_weight": route_weight, "w_gate": w_gate, "w_up": w_up, "w_down": w_down}


NORM_EPS = 1e-06
CLAMP_LIMIT = 7.0
SIGMOID_SCALE = 1.702

def slot_index(route_rows, expert_total, capacity):
    flat_ids = route_rows.reshape(-1)
    one_hot = (flat_ids[:, None] == jnp.arange(expert_total, dtype=jnp.int32)[None, :]).astype(jnp.int32)
    before = jnp.cumsum(one_hot, axis=0) - one_hot
    ranked = lax.optimization_barrier(jnp.sum(before * one_hot, axis=1))
    return (flat_ids * capacity + ranked).astype(jnp.int32)

def normed(tokens, norm_gain):
    values = tokens.astype(jnp.float32)
    scaled = values * lax.rsqrt(lax.optimization_barrier(jnp.mean(values * values, axis=-1, keepdims=True)) + NORM_EPS)
    return (scaled * norm_gain).astype(jnp.bfloat16)

def clamped_unit(gate_pre, up_pre):
    gated = jnp.minimum(gate_pre, CLAMP_LIMIT)
    upper = jnp.clip(up_pre, -CLAMP_LIMIT, CLAMP_LIMIT)
    return ((upper + 1.0) * gated * jax.nn.sigmoid(SIGMOID_SCALE * gated)).astype(jnp.bfloat16)

def reference(tokens, norm_gain, routing, route_weight, w_gate, w_up, w_down):
    normal = normed(tokens, norm_gain)
    dest = jax.vmap(lambda block_routes: slot_index(block_routes, EXPERTS, CAP))(routing.reshape(N_EP, TOK_DEV, TOP_K))
    slot_ids = jnp.arange(EXPERTS * CAP, dtype=jnp.int32)
    select = lax.optimization_barrier(jnp.sum(dest.reshape(N_EP, 1, TOK_DEV, TOP_K) == slot_ids[None, :, None, None], axis=3))
    sending = jnp.einsum('bst,btd->bsd', select.astype(jnp.float32), normal.reshape(N_EP, TOK_DEV, D).astype(jnp.float32)).astype(jnp.bfloat16)
    inbox = sending.reshape(N_EP, EXPERTS, CAP, D).transpose(1, 0, 2, 3).reshape(EXPERTS, N_EP * CAP, D)

    def expert(operands):
        rows_in, gate_mat, up_mat, down_mat = operands
        gate_pre = jnp.dot(rows_in, gate_mat, preferred_element_type=jnp.float32)
        up_pre = jnp.dot(rows_in, up_mat, preferred_element_type=jnp.float32)
        hidden = clamped_unit(gate_pre, up_pre)
        row_total = hidden.shape[0]
        partial_value = jnp.einsum('rjf,jfd->jrd', hidden.reshape(row_total, N_TP, FF // N_TP).astype(jnp.float32), down_mat.reshape(N_TP, FF // N_TP, D).astype(jnp.float32))
        rounded = lax.optimization_barrier(partial_value.astype(jnp.bfloat16))
        return lax.optimization_barrier(jnp.sum(rounded.astype(jnp.float32), axis=0)).astype(jnp.bfloat16)
    outbox = lax.map(expert, (inbox, w_gate, w_up, w_down))
    back = outbox.reshape(EXPERTS, N_EP, CAP, D).transpose(1, 0, 2, 3).reshape(N_EP, EXPERTS * CAP, D)
    picked = jnp.take_along_axis(back, dest[:, :, None], axis=1).reshape(TOKENS, TOP_K, D)
    mixed = lax.optimization_barrier(jnp.sum(picked.astype(jnp.float32) * route_weight[:, :, None], axis=1))
    return mixed.astype(jnp.bfloat16)
```

```python
import functools

import jax
import jax.numpy as jnp
from jax import lax
from jax.experimental import pallas as pl
from jax.experimental.pallas import tpu as pltpu
from jax.sharding import PartitionSpec as P

NORM_EPS = 1e-06
CLAMP_LIMIT = 7.0
SIGMOID_SCALE = 1.702
F32 = jnp.float32
BF16 = jnp.bfloat16
MESH = pl.DeviceIdType.MESH


def each(count, body):
    if count <= 8:
        for k in range(count):
            body(k)
    else:
        lax.fori_loop(0, count, lambda k, c: (body(k), c)[1], 0)


def kernel(
    n_ep, n_tp, tok_ref, gain_ref, route_ref, weight_ref, wg_hbm, wu_hbm, wd_hbm, out_ref,
    wg, wu, wd, acc_g, acc_u, sbuf, gbuf, part, din, ysend, yin, own, obuf, back,
    w_sem, a_send, a_recv, yf_send, yf_recv, cf_send, cf_recv, rl_send, rl_recv,
    d_send, d_recv, ys_send, ys_recv, b_send, b_recv,
):
    me = lax.axis_index("ep")
    j = lax.axis_index("tp")
    ny = n_tp // 2
    y, c = j // 2, j % 2
    core = y * 2 + (1 - c)
    toks, width = tok_ref.shape
    share = width // n_tp
    slot_rows = sbuf.shape[1]
    rows = n_ep * slot_rows
    top = route_ref.shape[1]
    others = [(y + d) % ny for d in range(1, ny)]
    order = [j, core] + [yy * 2 + c for yy in others] + [yy * 2 + (1 - c) for yy in others]
    aligned = share % 128 == 0

    def far(k):
        sign = 1 - 2 * (k % 2)
        return n_ep // 2 + sign * ((k + 1) // 2)

    def part_rows(s):
        start = s * share
        return pl.ds(pl.multiple_of(start, share) if not isinstance(start, int) else start, share)

    weight_copies = []
    for at, s in enumerate(order):
        cut = part_rows(s)
        pair = (
            pltpu.make_async_copy(wg_hbm.at[0, cut, :], wg.at[cut, :], w_sem.at[0, at]),
            pltpu.make_async_copy(wu_hbm.at[0, cut, :], wu.at[cut, :], w_sem.at[1, at]),
        )
        pair[0].start()
        pair[1].start()
        weight_copies.append(pair)

    down_order = []
    for yy in others + [y]:
        down_order += [yy * 2 + (1 - c), yy * 2 + c]
    down_copies = []
    if aligned:
        for at, s in enumerate(down_order):
            cut = part_rows(s)
            down_copies.append(
                pltpu.make_async_copy(wd_hbm.at[0, :, cut], wd.at[:, cut], w_sem.at[2, at])
            )
    else:
        down_copies.append(pltpu.make_async_copy(wd_hbm.at[0], wd, w_sem.at[2, 0]))
    for copy in down_copies:
        copy.start()

    barrier = pltpu.get_barrier_semaphore()

    def greet(k):
        pl.semaphore_signal(
            barrier, inc=1, device_id=((me + k + 1) % n_ep, j), device_id_type=MESH
        )

    each(n_ep - 1, greet)
    for peer in [core] + [yy * 2 + c for yy in others]:
        pl.semaphore_signal(barrier, inc=1, device_id=(me, peer), device_id_type=MESH)

    routes = route_ref[...]
    lanes = lax.broadcasted_iota(jnp.int32, (toks, 128), 1)
    chosen = jnp.zeros((toks, 128), F32)
    weights = jnp.zeros((toks, 128), F32)
    for k in range(top):
        hit = routes[:, k : k + 1] == lanes
        chosen += jnp.where(hit, 1.0, 0.0)
        weights += jnp.where(hit, weight_ref[:, k : k + 1], 0.0)
    before = lax.broadcasted_iota(jnp.int32, (toks, toks), 0) > lax.broadcasted_iota(
        jnp.int32, (toks, toks), 1
    )
    rank = jnp.dot(
        jnp.where(before, 1.0, 0.0).astype(BF16), chosen.astype(BF16), preferred_element_type=F32
    )
    r_row = lax.broadcasted_iota(jnp.int32, (rows, 128), 0)
    r_exp = lax.broadcasted_iota(jnp.int32, (rows, 128), 1)
    spread = jnp.where(r_row // slot_rows == r_exp, 1.0, 0.0).astype(BF16)
    nt = (((1,), (1,)), ((), ()))

    def across(a, b):
        return lax.dot_general(a, b, nt, preferred_element_type=F32)

    slot_a = (lax.broadcasted_iota(jnp.int32, (rows, toks), 0) % slot_rows).astype(F32)
    taken = across(spread, chosen.astype(BF16)) > 0.5
    select = jnp.where(
        taken & (across(spread, rank.astype(BF16)) == slot_a), 1.0, 0.0
    ).astype(BF16)

    values = tok_ref[...].astype(F32)
    scale = lax.rsqrt(jnp.mean(values * values, axis=-1, keepdims=True) + NORM_EPS)

    def put_share(tok_part, gain_part):
        normal = (tok_part.astype(F32) * scale * gain_part).astype(BF16)
        sending = jnp.dot(select, normal, preferred_element_type=F32).astype(BF16)
        sbuf[...] = sending.reshape(n_ep, slot_rows, share)

    if aligned:
        put_share(tok_ref[:, part_rows(j)], gain_ref[:, part_rows(j)])
    else:
        for s in range(n_tp):

            @pl.when(j == s)
            def _(s=s):
                cut = slice(s * share, (s + 1) * share)
                put_share(tok_ref[:, cut], gain_ref[:, cut])

    pl.semaphore_wait(barrier, n_ep - 1 + 1 + ny - 1)

    def a_copy(dst, src):
        return pltpu.make_async_remote_copy(
            src_ref=sbuf.at[dst], dst_ref=gbuf.at[j, src], send_sem=a_send.at[dst],
            recv_sem=a_recv.at[src], device_id=(dst, j), device_id_type=MESH,
        )

    def yf_copy(block, slot, yy, frm):
        return pltpu.make_async_remote_copy(
            src_ref=gbuf.at[slot, block], dst_ref=gbuf.at[slot, block],
            send_sem=yf_send.at[yy, block], recv_sem=yf_recv.at[frm, block],
            device_id=(me, yy * 2 + c), device_id_type=MESH,
        )

    def cf_copy(block, slot):
        return pltpu.make_async_remote_copy(
            src_ref=gbuf.at[slot, block], dst_ref=gbuf.at[slot, block],
            send_sem=cf_send.at[block], recv_sem=cf_recv.at[block],
            device_id=(me, core), device_id_type=MESH,
        )

    def rl_copy(slot, frm):
        return pltpu.make_async_remote_copy(
            src_ref=gbuf.at[slot], dst_ref=gbuf.at[slot], send_sem=rl_send.at[frm],
            recv_sem=rl_recv.at[frm], device_id=(me, core), device_id_type=MESH,
        )

    each(n_ep - 1, lambda k: a_copy((me + far(k)) % n_ep, me).start())
    gbuf[j, me] = sbuf[me]

    def forward(block):
        for yy in others:
            yf_copy(block, j, yy, y).start()
        cf_copy(block, j).start()

    forward(me)

    def arrive(k):
        src = (me + far(n_ep - 2 - k)) % n_ep
        a_copy(src, src).wait_recv()
        forward(src)

    each(n_ep - 1, arrive)

    place = across(weights.astype(BF16), spread)
    rest = weights - weights.astype(BF16).astype(F32)
    rest_place = across(rest.astype(BF16), spread)
    slot_b = (lax.broadcasted_iota(jnp.int32, (toks, rows), 1) % slot_rows).astype(F32)
    here = (across(rank.astype(BF16), spread) == slot_b) & (
        across(chosen.astype(BF16), spread) > 0.5
    )
    mix_high = jnp.where(here, place, 0.0).astype(BF16)
    mix_low = jnp.where(here, rest_place, 0.0).astype(BF16)

    def project(at):
        s = order[at]
        for copy in weight_copies[at]:
            copy.wait()
        piece = gbuf[s].reshape(rows, share)
        cut = part_rows(s)
        g = jnp.dot(piece, wg[cut, :], preferred_element_type=F32)
        u = jnp.dot(piece, wu[cut, :], preferred_element_type=F32)
        if at == 0:
            acc_g[...] = g
            acc_u[...] = u
        elif at < n_tp - 1:
            acc_g[...] += g
            acc_u[...] += u
        else:
            return acc_g[...] + g, acc_u[...] + u

    project(0)
    for yy in others:
        slot = yy * 2 + c
        each(n_ep, lambda b: yf_copy(b, slot, yy, yy).wait_recv())
        rl_copy(slot, yy).start()
    each(n_ep, lambda b: cf_copy(b, core).wait_recv())
    project(1)
    for at in range(2, 1 + ny):
        project(at)
    for at in range(1 + ny, n_tp):
        yy = others[at - 1 - ny]
        rl_copy(yy * 2 + (1 - c), yy).wait_recv()
        last = project(at)
    gate_pre, up_pre = last
    gated = jnp.minimum(gate_pre, CLAMP_LIMIT)
    upper = jnp.clip(up_pre, -CLAMP_LIMIT, CLAMP_LIMIT)
    hidden = ((upper + 1.0) * gated * jax.nn.sigmoid(SIGMOID_SCALE * gated)).astype(BF16)

    def d_copy(yy):
        return pltpu.make_async_remote_copy(
            src_ref=part.at[yy], dst_ref=din.at[yy], send_sem=d_send.at[yy],
            recv_sem=d_recv.at[yy], device_id=(me, core), device_id_type=MESH,
        )

    def ys_copy(block, yy, frm):
        return pltpu.make_async_remote_copy(
            src_ref=ysend.at[yy, block], dst_ref=yin.at[frm, block],
            send_sem=ys_send.at[yy, block], recv_sem=ys_recv.at[frm, block],
            device_id=(me, yy * 2 + c), device_id_type=MESH,
        )

    def b_copy(dst, src):
        return pltpu.make_async_remote_copy(
            src_ref=obuf.at[dst], dst_ref=back.at[src], send_sem=b_send.at[dst],
            recv_sem=b_recv.at[src], device_id=(dst, j), device_id_type=MESH,
        )

    def shaped(value):
        return value.reshape(n_ep, slot_rows, share)

    if aligned:

        def down(at):
            down_copies[at].wait()
            return jnp.dot(hidden, wd[:, part_rows(down_order[at])], preferred_element_type=F32)

        def close(done):
            d_copy(done).wait_recv()
            ysend[done] = (own[done].astype(F32) + din[done].astype(F32)).astype(BF16)
            each(n_ep, lambda k: ys_copy((me + far(k)) % n_ep, done, y).start())

        turn = others + [y]
        for i, yy in enumerate(turn):
            part[yy] = shaped(down(2 * i).astype(BF16))
            d_copy(yy).start()
            if i > 0:
                close(turn[i - 1])
            own[yy] = shaped(down(2 * i + 1).astype(BF16))
        d_copy(y).wait_recv()
    else:
        down_copies[0].wait()
        for s in range(n_tp):
            cut = slice(s * share, (s + 1) * share)
            value = shaped(jnp.dot(hidden, wd[:, cut], preferred_element_type=F32).astype(BF16))

            @pl.when(c == s % 2)
            def _(value=value, s=s):
                own[s // 2] = value

            @pl.when(c != s % 2)
            def _(value=value, s=s):
                part[s // 2] = value

        for yy in others + [y]:
            d_copy(yy).start()
        for yy in others + [y]:
            d_copy(yy).wait_recv()
            ysend[yy] = (own[yy].astype(F32) + din[yy].astype(F32)).astype(BF16)
        for yy in others:
            each(n_ep, lambda k: ys_copy((me + far(k)) % n_ep, yy, y).start())

    def finish(k):
        block = (me + far(k)) % n_ep
        total = own[y, block].astype(F32) + din[y, block].astype(F32)
        for yy in others:
            ys_copy(block, yy, yy).wait_recv()
            total += yin[yy, block].astype(F32)
        return block, total.astype(BF16)

    def finish_send(k):
        block, value = finish(k)
        obuf[block] = value
        b_copy(block, me).start()

    each(n_ep - 1, finish_send)
    _, value = finish(n_ep - 1)
    back[me] = value
    each(n_ep - 1, lambda k: b_copy((me + k + 1) % n_ep, (me + k + 1) % n_ep).wait_recv())
    returned = back[...].reshape(rows, share)
    mixed = jnp.dot(mix_high, returned, preferred_element_type=F32)
    mixed += jnp.dot(mix_low, returned, preferred_element_type=F32)
    out_ref[...] = mixed.astype(BF16)

    def drain(k):
        peer = (me + k + 1) % n_ep
        a_copy(peer, me).wait_send()
        b_copy(peer, me).wait_send()

    each(n_ep - 1, drain)

    def drain_blocks(b):
        cf_copy(b, j).wait_send()
        for yy in others:
            yf_copy(b, j, yy, y).wait_send()
            ys_copy(b, yy, y).wait_send()

    each(n_ep, drain_blocks)
    for yy in others:
        rl_copy(yy * 2 + c, yy).wait_send()
    for yy in others + [y]:
        d_copy(yy).wait_send()


def local(n_ep, n_tp, tokens, norm_gain, routing, route_weight, w_gate, w_up, w_down):
    toks, width = tokens.shape
    share = width // n_tp
    hidden = w_gate.shape[2]
    ny = n_tp // 2
    capacity = max(2, toks * routing.shape[1] // n_ep + 1)
    slot_rows = -(-capacity // 16) * 16
    rows = n_ep * slot_rows
    blocks = (n_ep, slot_rows, share)
    vmem = pl.BlockSpec(memory_space=pltpu.VMEM)
    hbm = pl.BlockSpec(memory_space=pl.ANY)
    dma = pltpu.SemaphoreType.DMA
    return pl.pallas_call(
        functools.partial(kernel, n_ep, n_tp),
        out_shape=jax.ShapeDtypeStruct((toks, share), BF16),
        in_specs=[vmem] * 4 + [hbm] * 3,
        out_specs=vmem,
        scratch_shapes=[
            pltpu.VMEM((width, hidden), BF16),
            pltpu.VMEM((width, hidden), BF16),
            pltpu.VMEM((hidden, width), BF16),
            pltpu.VMEM((rows, hidden), F32),
            pltpu.VMEM((rows, hidden), F32),
            pltpu.VMEM(blocks, BF16),
            pltpu.VMEM((n_tp,) + blocks, BF16),
            pltpu.VMEM((ny,) + blocks, BF16),
            pltpu.VMEM((ny,) + blocks, BF16),
            pltpu.VMEM((ny,) + blocks, BF16),
            pltpu.VMEM((ny,) + blocks, BF16),
            pltpu.VMEM((ny,) + blocks, BF16),
            pltpu.VMEM(blocks, BF16),
            pltpu.VMEM(blocks, BF16),
            dma((3, n_tp)),
            dma((n_ep,)), dma((n_ep,)),
            dma((ny, n_ep)), dma((ny, n_ep)),
            dma((n_ep,)), dma((n_ep,)),
            dma((ny,)), dma((ny,)),
            dma((ny,)), dma((ny,)),
            dma((ny, n_ep)), dma((ny, n_ep)),
            dma((n_ep,)), dma((n_ep,)),
        ],
        compiler_params=pltpu.CompilerParams(collective_id=0, has_side_effects=True),
    )(tokens, norm_gain.reshape(1, width), routing, route_weight, w_gate, w_up, w_down)


def solution(mesh):
    placed = (
        P("ep", None),
        P(),
        P("ep", None),
        P("ep", None),
        P("ep", None, "tp"),
        P("ep", None, "tp"),
        P("ep", "tp", None),
    )
    return jax.shard_map(
        functools.partial(local, mesh.shape["ep"], mesh.shape["tp"]),
        mesh=mesh, in_specs=placed, out_specs=P("ep", "tp"), check_vma=False,
    )
```

```python
import functools

import jax
import jax.numpy as jnp
from jax import lax
from jax.experimental import pallas as pl
from jax.experimental.pallas import tpu as pltpu
from jax.sharding import PartitionSpec as P

NORM_EPS = 1e-06
CLAMP_LIMIT = 7.0
SIGMOID_SCALE = 1.702
F32 = jnp.float32
BF16 = jnp.bfloat16
MESH = pl.DeviceIdType.MESH


def each(count, body):
    if count <= 8:
        for k in range(count):
            body(k)
    else:
        lax.fori_loop(0, count, lambda k, c: (body(k), c)[1], 0)


def kernel(
    n_ep, n_tp, tok_ref, gain_ref, route_ref, weight_ref, wg_hbm, wu_hbm, wd_hbm, out_ref,
    wg, wu, wd, acc_g, acc_u, sbuf, gbuf, part, din, ysend, yin, own, obuf, back,
    w_sem, a_send, a_recv, ag_send, ag_recv, yf_send, yf_recv, cf_send, cf_recv, rl_send, rl_recv,
    d_send, d_recv, ys_send, ys_recv, b_send, b_recv,
):
    me = lax.axis_index("ep")
    j = lax.axis_index("tp")
    ny = n_tp // 2
    y, c = j // 2, j % 2
    core = y * 2 + (1 - c)
    toks, width = tok_ref.shape
    share = width // n_tp
    slot_rows = sbuf.shape[2]
    rows = n_ep * slot_rows
    top = route_ref.shape[0]
    group = 4 if n_ep % 4 == 0 else 1
    base = me // group * group
    beyond = n_ep - group
    others = [(y + d) % ny for d in range(1, ny)]
    order = [j, core] + [yy * 2 + c for yy in others] + [yy * 2 + (1 - c) for yy in others]
    aligned = share % 128 == 0

    def far(k):
        sign = 1 - 2 * (k % 2)
        return n_ep // 2 + sign * ((k + 1) // 2)

    def part_rows(s):
        start = s * share
        return pl.ds(pl.multiple_of(start, share) if not isinstance(start, int) else start, share)

    weight_copies = []
    for at, s in enumerate(order):
        cut = part_rows(s)
        pair = (
            pltpu.make_async_copy(wg_hbm.at[0, cut, :], wg.at[cut, :], w_sem.at[0, at]),
            pltpu.make_async_copy(wu_hbm.at[0, cut, :], wu.at[cut, :], w_sem.at[1, at]),
        )
        pair[0].start()
        pair[1].start()
        weight_copies.append(pair)

    down_order = []
    for yy in others + [y]:
        down_order += [yy * 2 + (1 - c), yy * 2 + c]
    down_copies = []
    if aligned:
        for at, s in enumerate(down_order):
            cut = part_rows(s)
            down_copies.append(
                pltpu.make_async_copy(wd_hbm.at[0, :, cut], wd.at[:, cut], w_sem.at[2, at])
            )
    else:
        down_copies.append(pltpu.make_async_copy(wd_hbm.at[0], wd, w_sem.at[2, 0]))
    for copy in down_copies:
        copy.start()

    barrier = pltpu.get_barrier_semaphore()

    def greet(k):
        pl.semaphore_signal(
            barrier, inc=1, device_id=((me + k + 1) % n_ep, j), device_id_type=MESH
        )

    each(n_ep - 1, greet)
    for peer in [core] + [yy * 2 + c for yy in others]:
        pl.semaphore_signal(barrier, inc=1, device_id=(me, peer), device_id_type=MESH)

    routes = route_ref[...]
    experts = lax.broadcasted_iota(jnp.int32, (128, toks), 0)
    chosen = jnp.zeros((128, toks), F32)
    weights = jnp.zeros((128, toks), F32)
    for k in range(top):
        hit = routes[k : k + 1, :] == experts
        chosen += jnp.where(hit, 1.0, 0.0)
        weights += jnp.where(hit, weight_ref[k : k + 1, :], 0.0)
    before = lax.broadcasted_iota(jnp.int32, (toks, toks), 0) < lax.broadcasted_iota(
        jnp.int32, (toks, toks), 1
    )
    chosen = chosen.astype(BF16)
    rank = jnp.dot(chosen, jnp.where(before, 1.0, 0.0).astype(BF16), preferred_element_type=F32)
    r_row = lax.broadcasted_iota(jnp.int32, (rows, 128), 0)
    r_exp = lax.broadcasted_iota(jnp.int32, (rows, 128), 1)
    spread = jnp.where(r_row // slot_rows == r_exp, 1.0, 0.0).astype(BF16)

    def spread_out(a):
        return jnp.dot(spread, a.astype(BF16), preferred_element_type=F32)

    slot = (lax.broadcasted_iota(jnp.int32, (rows, toks), 0) % slot_rows).astype(F32)
    here = (spread_out(chosen) > 0.5) & (spread_out(rank) == slot)
    select = jnp.where(here, 1.0, 0.0).astype(BF16)

    values = tok_ref[...].astype(F32)
    scale = lax.rsqrt(jnp.mean(values * values, axis=-1, keepdims=True) + NORM_EPS)

    def put_share(at, tok_part, gain_part):
        normal = (tok_part.astype(F32) * scale * gain_part).astype(BF16)
        sending = jnp.dot(select, normal, preferred_element_type=F32).astype(BF16)
        sbuf[at] = sending.reshape(n_ep, slot_rows, share)

    if aligned:
        for yy in [y] + others:
            cut = part_rows(yy * 2 + c)
            put_share(yy, tok_ref[:, cut], gain_ref[:, cut])
    else:
        for s in range(n_tp):

            @pl.when(c == s % 2)
            def _(s=s):
                cut = slice(s * share, (s + 1) * share)
                put_share(s // 2, tok_ref[:, cut], gain_ref[:, cut])

    pl.semaphore_wait(barrier, n_ep - 1 + 1 + ny - 1)

    def a_copy(dst, src):
        return pltpu.make_async_remote_copy(
            src_ref=sbuf.at[y, dst], dst_ref=gbuf.at[j, src], send_sem=a_send.at[dst],
            recv_sem=a_recv.at[src], device_id=(dst, j), device_id_type=MESH,
        )

    def ag_copy(dst, src, yy):
        return pltpu.make_async_remote_copy(
            src_ref=sbuf.at[yy, dst], dst_ref=gbuf.at[yy * 2 + c, src],
            send_sem=ag_send.at[yy, dst], recv_sem=ag_recv.at[yy, src],
            device_id=(dst, j), device_id_type=MESH,
        )

    def yf_copy(block, slot, yy, frm):
        return pltpu.make_async_remote_copy(
            src_ref=gbuf.at[slot, block], dst_ref=gbuf.at[slot, block],
            send_sem=yf_send.at[yy, block], recv_sem=yf_recv.at[frm, block],
            device_id=(me, yy * 2 + c), device_id_type=MESH,
        )

    def cf_copy(block, slot):
        return pltpu.make_async_remote_copy(
            src_ref=gbuf.at[slot, block], dst_ref=gbuf.at[slot, block],
            send_sem=cf_send.at[block], recv_sem=cf_recv.at[block],
            device_id=(me, core), device_id_type=MESH,
        )

    def rl_copy(slot, frm):
        return pltpu.make_async_remote_copy(
            src_ref=gbuf.at[slot], dst_ref=gbuf.at[slot], send_sem=rl_send.at[frm],
            recv_sem=rl_recv.at[frm], device_id=(me, core), device_id_type=MESH,
        )

    def outer(k):
        return (base + group + (me - base + k) % beyond) % n_ep

    near = [base + (me - base + d) % group for d in range(1, group)]
    if beyond:
        each(beyond, lambda k: a_copy(outer(k), me).start())
    for dst in near:
        a_copy(dst, me).start()
    for yy in others:
        for dst in near:
            ag_copy(dst, me, yy).start()
    for yy in [y] + others:
        gbuf[yy * 2 + c, me] = sbuf[yy, me]
    cf_copy(me, j).start()

    def arrive(k):
        src = outer(k)
        a_copy(src, src).wait_recv()
        for yy in others:
            yf_copy(src, j, yy, y).start()
        cf_copy(src, j).start()

    if beyond:
        each(beyond, arrive)
    for src in near:
        a_copy(src, src).wait_recv()
        cf_copy(src, j).start()

    high = weights.astype(BF16)
    mix_high = jnp.where(here, spread_out(high), 0.0).astype(BF16)
    mix_low = jnp.where(here, spread_out(weights - high.astype(F32)), 0.0).astype(BF16)

    def project(at):
        s = order[at]
        for copy in weight_copies[at]:
            copy.wait()
        piece = gbuf[s].reshape(rows, share)
        cut = part_rows(s)
        g = jnp.dot(piece, wg[cut, :], preferred_element_type=F32)
        u = jnp.dot(piece, wu[cut, :], preferred_element_type=F32)
        if at == 0:
            acc_g[...] = g
            acc_u[...] = u
        elif at < n_tp - 1:
            acc_g[...] += g
            acc_u[...] += u
        else:
            return acc_g[...] + g, acc_u[...] + u

    project(0)
    for yy in others:
        for src in near:
            ag_copy(src, src, yy).wait_recv()
        if beyond:
            each(beyond, lambda k: yf_copy(outer(k), yy * 2 + c, yy, yy).wait_recv())
        rl_copy(yy * 2 + c, yy).start()
    each(n_ep, lambda b: cf_copy(b, core).wait_recv())
    project(1)
    for at in range(2, 1 + ny):
        project(at)
    for at in range(1 + ny, n_tp):
        yy = others[at - 1 - ny]
        rl_copy(yy * 2 + (1 - c), yy).wait_recv()
        last = project(at)
    gate_pre, up_pre = last
    gated = jnp.minimum(gate_pre, CLAMP_LIMIT)
    upper = jnp.clip(up_pre, -CLAMP_LIMIT, CLAMP_LIMIT)
    hidden = ((upper + 1.0) * gated * jax.nn.sigmoid(SIGMOID_SCALE * gated)).astype(BF16)

    def d_copy(yy):
        return pltpu.make_async_remote_copy(
            src_ref=part.at[yy], dst_ref=din.at[yy], send_sem=d_send.at[yy],
            recv_sem=d_recv.at[yy], device_id=(me, core), device_id_type=MESH,
        )

    def ys_copy(block, yy, frm):
        return pltpu.make_async_remote_copy(
            src_ref=ysend.at[yy, block], dst_ref=yin.at[frm, block],
            send_sem=ys_send.at[yy, block], recv_sem=ys_recv.at[frm, block],
            device_id=(me, yy * 2 + c), device_id_type=MESH,
        )

    def b_copy(dst, src):
        return pltpu.make_async_remote_copy(
            src_ref=obuf.at[dst], dst_ref=back.at[src], send_sem=b_send.at[dst],
            recv_sem=b_recv.at[src], device_id=(dst, j), device_id_type=MESH,
        )

    def shaped(value):
        return value.reshape(n_ep, slot_rows, share)

    if aligned:

        def down(at):
            down_copies[at].wait()
            return jnp.dot(hidden, wd[:, part_rows(down_order[at])], preferred_element_type=F32)

        def close(done):
            d_copy(done).wait_recv()
            ysend[done] = (own[done].astype(F32) + din[done].astype(F32)).astype(BF16)
            each(n_ep, lambda k: ys_copy((me + far(k)) % n_ep, done, y).start())

        turn = others + [y]
        for i, yy in enumerate(turn):
            part[yy] = shaped(down(2 * i).astype(BF16))
            d_copy(yy).start()
            if i > 0:
                close(turn[i - 1])
            own[yy] = shaped(down(2 * i + 1).astype(BF16))
        d_copy(y).wait_recv()
    else:
        down_copies[0].wait()
        for s in range(n_tp):
            cut = slice(s * share, (s + 1) * share)
            value = shaped(jnp.dot(hidden, wd[:, cut], preferred_element_type=F32).astype(BF16))

            @pl.when(c == s % 2)
            def _(value=value, s=s):
                own[s // 2] = value

            @pl.when(c != s % 2)
            def _(value=value, s=s):
                part[s // 2] = value

        for yy in others + [y]:
            d_copy(yy).start()
        for yy in others + [y]:
            d_copy(yy).wait_recv()
            ysend[yy] = (own[yy].astype(F32) + din[yy].astype(F32)).astype(BF16)
        for yy in others:
            each(n_ep, lambda k: ys_copy((me + far(k)) % n_ep, yy, y).start())

    def finish(k):
        block = (me + far(k)) % n_ep
        total = own[y, block].astype(F32) + din[y, block].astype(F32)
        for yy in others:
            ys_copy(block, yy, yy).wait_recv()
            total += yin[yy, block].astype(F32)
        return block, total.astype(BF16)

    def finish_send(k):
        block, value = finish(k)
        obuf[block] = value
        b_copy(block, me).start()

    each(n_ep - 1, finish_send)
    _, value = finish(n_ep - 1)
    back[me] = value
    each(n_ep - 1, lambda k: b_copy((me + k + 1) % n_ep, (me + k + 1) % n_ep).wait_recv())
    returned = back[...].reshape(rows, share)
    over_rows = (((0,), (0,)), ((), ()))
    mixed = lax.dot_general(mix_high, returned, over_rows, preferred_element_type=F32)
    mixed += lax.dot_general(mix_low, returned, over_rows, preferred_element_type=F32)
    out_ref[...] = mixed.astype(BF16)

    def drain(k):
        peer = (me + k + 1) % n_ep
        a_copy(peer, me).wait_send()
        b_copy(peer, me).wait_send()

    each(n_ep - 1, drain)

    def drain_blocks(b):
        cf_copy(b, j).wait_send()
        for yy in others:
            ys_copy(b, yy, y).wait_send()

    each(n_ep, drain_blocks)
    for yy in others:
        if beyond:
            each(beyond, lambda k: yf_copy(outer(k), j, yy, y).wait_send())
        for dst in near:
            ag_copy(dst, me, yy).wait_send()
    for yy in others:
        rl_copy(yy * 2 + c, yy).wait_send()
    for yy in others + [y]:
        d_copy(yy).wait_send()


def local(n_ep, n_tp, tokens, norm_gain, routing, route_weight, w_gate, w_up, w_down):
    toks, width = tokens.shape
    share = width // n_tp
    hidden = w_gate.shape[2]
    ny = n_tp // 2
    capacity = max(2, toks * routing.shape[1] // n_ep + 1)
    slot_rows = -(-capacity // 16) * 16
    rows = n_ep * slot_rows
    blocks = (n_ep, slot_rows, share)
    vmem = pl.BlockSpec(memory_space=pltpu.VMEM)
    hbm = pl.BlockSpec(memory_space=pl.ANY)
    dma = pltpu.SemaphoreType.DMA
    return pl.pallas_call(
        functools.partial(kernel, n_ep, n_tp),
        out_shape=jax.ShapeDtypeStruct((toks, share), BF16),
        in_specs=[vmem] * 4 + [hbm] * 3,
        out_specs=vmem,
        scratch_shapes=[
            pltpu.VMEM((width, hidden), BF16),
            pltpu.VMEM((width, hidden), BF16),
            pltpu.VMEM((hidden, width), BF16),
            pltpu.VMEM((rows, hidden), F32),
            pltpu.VMEM((rows, hidden), F32),
            pltpu.VMEM((ny,) + blocks, BF16),
            pltpu.VMEM((n_tp,) + blocks, BF16),
            pltpu.VMEM((ny,) + blocks, BF16),
            pltpu.VMEM((ny,) + blocks, BF16),
            pltpu.VMEM((ny,) + blocks, BF16),
            pltpu.VMEM((ny,) + blocks, BF16),
            pltpu.VMEM((ny,) + blocks, BF16),
            pltpu.VMEM(blocks, BF16),
            pltpu.VMEM(blocks, BF16),
            dma((3, n_tp)),
            dma((n_ep,)), dma((n_ep,)),
            dma((ny, n_ep)), dma((ny, n_ep)),
            dma((ny, n_ep)), dma((ny, n_ep)),
            dma((n_ep,)), dma((n_ep,)),
            dma((ny,)), dma((ny,)),
            dma((ny,)), dma((ny,)),
            dma((ny, n_ep)), dma((ny, n_ep)),
            dma((n_ep,)), dma((n_ep,)),
        ],
        compiler_params=pltpu.CompilerParams(collective_id=0, has_side_effects=True),
    )(tokens, norm_gain.reshape(1, width), routing.T, route_weight.T, w_gate, w_up, w_down)


def solution(mesh):
    placed = (
        P("ep", None),
        P(),
        P("ep", None),
        P("ep", None),
        P("ep", None, "tp"),
        P("ep", None, "tp"),
        P("ep", "tp", None),
    )
    return jax.shard_map(
        functools.partial(local, mesh.shape["ep"], mesh.shape["tp"]),
        mesh=mesh, in_specs=placed, out_specs=P("ep", "tp"), check_vma=False,
    )
```
